256 devices in a mesh: grp: 2 (over y), sp: 16 (over z), tp: 8 (over x, core).
Axes of the slice: x: 4, y: 2, z: 16, core: 2. Of those that a mesh axis runs over, the one named last changes fastest.
The devices are a block of a 4x16x16 slice.
Arguments:
- stream: bfloat16 [98304, 4096], P(('grp', 'sp', 'tp')), parts along dimension 0, may hold values from -6 to 6
- norm_gain: float32 [2, 4096], replicated, may hold values from 0.1 to 1.9
- mix_weight: bfloat16 [2, 4, 1024, 1024], P(None, None, 'sp', 'tp'), may hold values from -0.1875 to 0.1875
- branch_scale: float32 [2, 4096], replicated, may hold values from 0.1 to 1.9
Outputs:
- result: bfloat16 [98304, 4096], P(('grp', 'sp', 'tp')), parts along dimension 0
The draws below stay inside these ranges and needn't reach their ends.
There are 2 independent parts, one for each index of `grp`. The reference program is written for one: setup_inputs(seed, part) draws one part's arguments, and reference() takes and returns one part's arrays. A program takes and returns all parts, laid end to end along the dimension named above; an argument that names none is the same for every part. Nothing has to cross between parts.
All inputs are finite; a program needn't handle non-finite values.
Results may differ from the reference program's by a relative error of at most 0.0056.
Values may be sent and summed in bfloat16 or wider, within the bound.
No kernel may reach another device: no remote copies, remote signals or barrier semaphores. Data moves between devices by JAX's collectives and lax.ppermute only.
A program may use at most 128 MiB of HBM per device.

```python
import jax
import jax.numpy as jnp
from jax import lax

GW = 1024
G = 4
D = 4096
LAYERS = 2
TOKENS = 49152


def block_scale(own_key, shape, split, low, top_value):
    factor_of = 1.0
    for axis_at, blocks in split:
        steps = jax.random.uniform(jax.random.fold_in(jax.random.fold_in(own_key, 6), axis_at), (blocks,), jnp.float32, low / len(split), top_value / len(split))
        factor_of = factor_of * jnp.repeat(jnp.exp(steps), shape[axis_at] // blocks).reshape((-1,) + (1,) * (len(shape) - 1 - axis_at))
    return factor_of


def gaussian(key, shape, scale, bound, cuts=(), kind=jnp.bfloat16):
    loudness = block_scale(key, shape, cuts, -0.22, 0.18) if cuts else 1.0
    values = jax.random.normal(key, shape, jnp.float32) * scale * loudness
    return jnp.minimum(jnp.maximum(values, -bound), bound).astype(kind)


def setup_inputs(seed: int = 0, part: int = 0) -> dict:
    streams_of = jax.random.split(jax.random.key(seed), 5)
    part_splits = jax.random.split(jax.random.fold_in(streams_of[4], part), 5)
    stream = gaussian(part_splits[0], (TOKENS, D), 1.0, 6.0, ((0, 128),))
    norm_gain = jnp.clip(1.0 + 0.18 * jax.random.normal(streams_of[1], (LAYERS, D), jnp.float32), 0.1, 1.9)
    mix_weight = gaussian(streams_of[2], (LAYERS, G, GW, GW), GW ** -0.5, 0.1875, ((2, 16), (3, 8)))
    branch_scale = jnp.clip(1.0 + 0.18 * jax.random.normal(streams_of[3], (LAYERS, D), jnp.float32), 0.1, 1.9)
    return dict(stream=stream, norm_gain=norm_gain, mix_weight=mix_weight, branch_scale=branch_scale)


epsilon = 1e-06
window_lengths = (2, 4, 8, 16)

def trailing_sum(group_block, window_len):
    running = group_block
    for back_step in range(1, window_len):
        shifted = jnp.concatenate([jnp.zeros((back_step, group_block.shape[1]), jnp.float32), group_block[:-back_step]], axis=0)
        running = running + shifted
    return running

def reference(stream, norm_gain, mix_weight, branch_scale):
    residual = stream.astype(jnp.float32)
    counts_base = jnp.arange(TOKENS, dtype=jnp.float32) + 1.0
    for layer_idx in range(LAYERS):
        scale_rows = lax.rsqrt(lax.optimization_barrier(jnp.mean(residual * residual, axis=1, keepdims=True)) + epsilon)
        normed = (residual * scale_rows * norm_gain[layer_idx]).astype(jnp.bfloat16)
        outputs = []
        for group_idx in range(G):
            window_len = window_lengths[group_idx]
            group_block = normed[:, group_idx * GW:(group_idx + 1) * GW].astype(jnp.float32)
            window_mean = trailing_sum(group_block, window_len) / jnp.minimum(counts_base, float(window_len))[:, None]
            pooled = (window_mean - group_block).astype(jnp.bfloat16)
            outputs.append(jnp.dot(pooled, mix_weight[layer_idx, group_idx], preferred_element_type=jnp.float32))
        residual = residual + jnp.concatenate(outputs, axis=1) * branch_scale[layer_idx]
    return residual.astype(jnp.bfloat16)
```

```python
import functools

import jax
import jax.numpy as jnp
from jax import lax
from jax.experimental import pallas as pl
from jax.experimental.pallas import tpu as pltpu
from jax.sharding import PartitionSpec as P


GW = 1024
G = 4
D = G * GW
EPS = 1e-06
WINDOWS = (2, 4, 8, 16)
HALO = 16
LAYERS = 2
CORES = 2
NZ = 16
NX = 4


OFFSETS = (4, 0, -4, -8, 3, -1, -5, -9, 5, 1, -3, -7, -2, -6, 6, 2)
SHARED = (0,)
COMMON = 2

CHIPS = (("h", 0), ("o", 2), ("l", 3), ("r", 1))


def issued(v, axis, route):
    n = lax.axis_size(axis)
    return lax.ppermute(v, axis, [(i, route(i, n)) for i in range(n)])


def shift_sp(v, distance):
    return issued(v, "sp", lambda i, n: (i + distance) % n)


def shift_x(v, distance):
    return issued(v, "tp", lambda i, n: (i + CORES * distance) % n)


def swap_core(v):
    return issued(v, "tp", lambda i, n: i ^ 1)


def swap_grp(v):
    return issued(v, "grp", lambda i, n: i ^ 1)


def join(layout, *arrays):
    shapes = []
    for out in layout:
        parts = [jax.eval_shape(lambda v, cut=cut: cut(v), arrays[i]) for i, cut in out]
        shapes.append(jax.ShapeDtypeStruct((sum(p.shape[0] for p in parts), *parts[0].shape[1:]), parts[0].dtype))

    def body(*refs):
        for out, ref in zip(layout, refs[len(arrays) :]):
            at = 0
            for i, cut in out:
                v = cut(refs[i])
                ref[at : at + v.shape[0]] = v
                at += v.shape[0]

    out = pl.pallas_call(
        body, out_shape=tuple(shapes), in_specs=[VMEM] * len(arrays), out_specs=tuple(VMEM for _ in shapes)
    )(*arrays)
    return out


def take(*index):
    return lambda v: v[index if len(index) > 1 else index[0]]


VMEM = pl.BlockSpec(memory_space=pltpu.VMEM)
HBM = pl.BlockSpec(memory_space=pltpu.HBM)
MIB = 1024 * 1024


def gather(piece):
    up, down, far = shift_sp(piece, 4), shift_sp(piece, -4), shift_sp(piece, 8)
    sets = join(
        [
            [(i, take(slice(layer, layer + 1))) for i in places]
            for layer in range(LAYERS)
            for places in ((0, 1, 2, 3), (1, 2), (0, 1))
        ],
        down, piece, up, far,
    )
    layers = []
    for layer in range(LAYERS):
        s, s1, s2 = sets[3 * layer : 3 * layer + 3]
        near = [s] + [shift_sp(v, d) for v, d in ((s, 1), (s, -1), (s1, 2), (s2, -2))]
        shared = layer in SHARED
        home, mine, *cut = join_halves(shared, *near)
        opposite = shift_x(mine, 2)
        own = {"h": home, "o": opposite, "yo": swap_grp(opposite)}
        for name, distance in (("l", 1), ("r", -1)):
            if shared:
                common, half = cut
                half = shift_x(half, distance)
                own |= {name + "c": shift_x(common, distance), name + "e": half}
                own["y" + name + "e"] = swap_grp(half)
            else:
                own[name] = shift_x(home, distance)
        theirs = {n: swap_core(v) for n, v in own.items()}
        layers.append((tuple(own), [*own.values(), *theirs.values()]))
    return layers


def join_halves(shared, *arrays):
    n = sum(v.shape[0] for v in arrays)
    slots, rest = arrays[0].shape[1], arrays[0].shape[2:]

    def body(*refs):
        whole, mine, *cut = refs[len(arrays) :]
        at = 0
        for r in refs[: len(arrays)]:
            whole[at : at + r.shape[0]] = r[...]
            at += r.shape[0]
        mine[...] = whole[pl.ds((lax.axis_index("grp") % 2) * (n // 2), n // 2)]
        if shared:
            cut[0][...] = whole[:, :COMMON]
            cut[1][...] = mine[:, COMMON:]

    sizes = [(n, slots), (n // 2, slots)] + [(n, COMMON), (n // 2, slots - COMMON)] * shared
    shapes = tuple(jax.ShapeDtypeStruct((*m, *rest), arrays[0].dtype) for m in sizes)
    return pl.pallas_call(
        body, out_shape=shapes, in_specs=[VMEM] * len(arrays), out_specs=(VMEM,) * len(shapes)
    )(*arrays)


def position():
    tp = lax.axis_index("tp")
    return lax.axis_index("sp"), tp // CORES, tp % CORES


def first_row(rows):
    return (lax.axis_index("sp") * lax.axis_size("tp") + lax.axis_index("tp")) * rows


def norm_rows(load, gain_ref, n_ref, base, rows):
    def step(i, _):
        r = pl.multiple_of(i * 16, 16)
        v = load(r)
        scale = lax.rsqrt(jnp.sum(v * v, axis=1, keepdims=True) * (1.0 / D) + EPS)
        n_ref[pl.ds(base + r, 16), :] = (v * scale * gain_ref[0:1, :]).astype(jnp.bfloat16)
        return 0

    lax.fori_loop(0, rows // 16, step, 0, unroll=2)


def pool_rows(get, out_ref, rows, block, first):
    sp = position()[0]
    chunk = sp // 2
    odd = jnp.full((block, 128), sp % 2, jnp.int32) == 1
    low = lax.broadcasted_iota(jnp.int32, (block, 128), 1) < 64
    for g, window in enumerate(WINDOWS):

        def step(i, _, g=g, window=window):
            r = pl.multiple_of(i * block, 16)
            pos = first + r + lax.broadcasted_iota(jnp.int32, (block, 1), 0)
            inv = 1.0 / jnp.clip(pos + 1, 1, window).astype(jnp.float32)
            plain, turned = [], []
            for t in range(8):
                c = pl.multiple_of(g * GW + ((chunk + t) % 8) * 128, 128)
                v = get(r, block + HALO, c)
                s, d = v, 1
                while d < window:
                    s = s + pltpu.roll(s, d, 0)
                    d *= 2
                p = s[HALO:] * inv - v[HALO:]
                plain.append(p)
                turned.append(pltpu.roll(p, 64, 1))
            for t in range(8):
                o = jnp.where(odd, jnp.where(low, turned[t], turned[(t + 1) % 8]), plain[t])
                out_ref[pl.ds(r, block), g * GW + t * 128 : g * GW + (t + 1) * 128] = o.astype(jnp.bfloat16)
            return 0

        lax.fori_loop(0, rows // block, step, 0)


def fetch(names, parts, buffers, sems):
    waits = {n: [] for n in names}
    for i, (part, buffer) in enumerate(zip(parts, buffers)):
        copy = pltpu.make_async_copy(part, buffer, sems.at[i])
        copy.start()
        waits[names[i % len(names)]].append(copy)
    return waits


def mix(pooled_ref, names, buffers, waits, emit, start=None, finish=None, unroll=False):
    place = {o % NZ: k for k, o in enumerate(OFFSETS)}
    half = NZ // 2
    _, chip, own = position()
    odd = jnp.full((GW // NZ, 128), lax.axis_index("grp") % 2, jnp.int32) == 1
    held = [dict(zip(names, buffers[dc * len(names) :])) for dc in range(CORES)]

    def weight(name, dc, g, k, common):
        refs = held[dc]
        if name + "c" in refs:
            if common:
                return refs[name + "c"][k, g]
            name, g = name + "e", g - COMMON
        if "y" + name not in refs:
            return refs[name][k, g]
        brought, peers = refs[name][k % half, g], refs["y" + name][k % half, g]
        return jnp.where(odd, peers, brought) if k < half else jnp.where(odd, brought, peers)

    for name, dx in CHIPS:
        if not any(name in n for n in names):
            continue
        for n in names:
            if name in n:
                for copy in waits[n]:
                    copy.wait()
        if start:
            start(name)
        x = (chip + dx) % NX

        def group(g, common, name=name, x=x):
            cols = [jnp.concatenate([weight(name, dc, g, place[j], common) for j in range(NZ)], axis=0) for dc in range(CORES)]
            lhs = pooled_ref[:, pl.ds(pl.multiple_of(g * GW, GW), GW)]
            m = jnp.dot(lhs, jnp.concatenate(cols, axis=1), preferred_element_type=jnp.float32)
            at = pl.multiple_of(g * GW + x * 256, 256)
            emit(name, g, at, [(pl.multiple_of((own + dc) % CORES * 128, 128), m[:, dc * 128 : (dc + 1) * 128]) for dc in range(CORES)])

        for lo, hi in ((0, COMMON), (COMMON, G)) if name + "c" in names else ((0, G),):
            if unroll:
                for g in range(lo, hi):
                    group(g, hi == COMMON)
            else:
                lax.fori_loop(lo, hi, lambda g, _: group(g, hi == COMMON), None)
        if finish:
            finish(name)


def pool_kernel(halo_ref, gain_ref, stream_hbm, out_hbm, stream_ref, out_ref, n_ref, sems):
    rows = stream_ref.shape[0]
    read = pltpu.make_async_copy(stream_hbm, stream_ref, sems.at[0])
    read.start()
    norm_rows(lambda r: halo_ref[pl.ds(r, 16), :].astype(jnp.float32), gain_ref, n_ref, 0, 2 * HALO)
    read.wait()
    norm_rows(lambda r: stream_ref[pl.ds(r, 16), :].astype(jnp.float32), gain_ref, n_ref, 2 * HALO, rows)
    pool_rows(
        lambda r, n, c: n_ref[pl.ds(r, n), pl.ds(c, 128)].astype(jnp.float32), out_ref, rows + HALO, 80, first_row(rows) - HALO
    )
    write = pltpu.make_async_copy(out_ref, out_hbm, sems.at[1])
    write.start()
    write.wait()


def middle_kernel(names, halo_ref, stream_ref, pooled_ref, scale_ref, gain_ref, *rest):
    n = CORES * len(names)
    parts, (res_out, pooled_out), (r_ref, square_ref, norm_ref, out_sems) = rest[:n], rest[n : n + 2], rest[n + 2 : n + 6]
    buffers, sems = rest[n + 6 : -1], rest[-1]
    waits = fetch(names, parts, buffers, sems)
    rows = stream_ref.shape[0]
    square_ref[...] = jnp.zeros_like(square_ref)
    copies = {}
    for i, (name, dx) in enumerate(CHIPS):
        at = [pl.multiple_of(g * GW + (position()[1] + dx) % NX * 256, 256) for g in range(G)]
        copies[name] = [
            pltpu.make_async_copy(r_ref.at[pl.ds(HALO, rows), pl.ds(c, 256)], res_out.at[:, pl.ds(c, 256)], out_sems.at[i * G + g])
            for g, c in enumerate(at)
        ]

    def emit(name, g, at, pieces):
        for shift, m in pieces:
            cols = pl.ds(at + shift, 128)
            m = m * scale_ref[0:1, cols]
            top = halo_ref[HALO:, cols].astype(jnp.float32) + m[:HALO]
            body = stream_ref[:, cols].astype(jnp.float32) + m[HALO:]
            r_ref[:HALO, cols] = top
            r_ref[HALO:, cols] = body
            square_ref[:HALO] += top * top
            square_ref[HALO:] += body * body

    def finish(name):
        for copy in copies[name]:
            copy.start()

    mix(pooled_ref, names, buffers, waits, emit, finish=finish, unroll=True)
    scale = lax.rsqrt(jnp.sum(square_ref[...], axis=1, keepdims=True) * (1.0 / D) + EPS)
    norm_ref[...] = jnp.broadcast_to(scale, norm_ref.shape)

    def get(r, n, c):
        cols = pl.ds(c, 128)
        v = r_ref[pl.ds(r, n), cols] * norm_ref[pl.ds(r, n), :] * gain_ref[1:2, cols]
        return v.astype(jnp.bfloat16).astype(jnp.float32)

    pool_rows(get, pooled_out, rows, 96, first_row(rows))
    for name, _ in CHIPS:
        for copy in copies[name]:
            copy.wait()


def last_kernel(names, res_ref, pooled_ref, scale_ref, *rest):
    n = CORES * len(names)
    parts, rest = rest[:n], rest[len(rest) - 5 - n :]
    out_ref, r_ref, o_ref, in_sems, out_sems = rest[0], rest[1], rest[2], rest[3], rest[4]
    buffers, sems = rest[5:], in_sems
    chip = position()[1]
    used = [(name, dx) for name, dx in CHIPS if any(name in n for n in names)]
    waits = fetch(names, parts, buffers, sems)
    reads, writes = [], []
    for i, (_, dx) in enumerate(used):
        for g in range(G):
            cols = pl.ds(pl.multiple_of(g * GW + (chip + dx) % NX * 256, 256), 256)
            k = i * G + g
            reads.append(pltpu.make_async_copy(res_ref.at[:, cols], r_ref.at[k], in_sems.at[n + k]))
            writes.append(pltpu.make_async_copy(o_ref.at[k], out_ref.at[:, cols], out_sems.at[k]))
    for copy in reads:
        copy.start()
    first = {name: i * G for i, (name, _) in enumerate(used)}

    def start(name):
        for copy in reads[first[name] : first[name] + G]:
            copy.wait()

    def finish(name):
        for copy in writes[first[name] : first[name] + G]:
            copy.start()

    def emit(name, g, at, pieces):
        k = first[name] + g
        for shift, m in pieces:
            cols = pl.ds(shift, 128)
            o_ref[k, :, cols] = (r_ref[k, :, cols] + m * scale_ref[1:2, pl.ds(at + shift, 128)]).astype(jnp.bfloat16)

    mix(pooled_ref, names, buffers, waits, emit, start, finish)
    for copy in writes:
        copy.wait()


def last_call(residual, pooled, scale, names, parts, before):
    rows = residual.shape[0]
    blocks = G * sum(any(c in n for n in names) for c, _ in CHIPS)
    more = [] if before is None else [before]
    return pl.pallas_call(
        functools.partial(last_kernel, names),
        out_shape=jax.ShapeDtypeStruct((rows, D), jnp.bfloat16),
        in_specs=[HBM, VMEM, VMEM] + [HBM] * (len(parts) + len(more)),
        out_specs=HBM,
        scratch_shapes=[
            pltpu.VMEM((blocks, rows, 256), jnp.float32),
            pltpu.VMEM((blocks, rows, 256), jnp.bfloat16),
            pltpu.SemaphoreType.DMA((len(parts) + blocks,)),
            pltpu.SemaphoreType.DMA((blocks,)),
        ]
        + [pltpu.VMEM(v.shape, v.dtype) for v in parts],
        input_output_aliases={3 + len(parts): 0} if more else {},
        compiler_params=pltpu.CompilerParams(vmem_limit_bytes=24 * MIB),
    )(residual, pooled, scale, *parts, *more)


def call(kernel, out_shape, out_specs, args, scratch, limit, names=(), parts=()):
    if names:
        kernel = functools.partial(kernel, names)
        scratch = scratch + [pltpu.VMEM(v.shape, v.dtype) for v in parts] + [pltpu.SemaphoreType.DMA((len(parts),))]
    return pl.pallas_call(
        kernel,
        out_shape=out_shape,
        in_specs=[VMEM] * len(args) + [HBM] * len(parts),
        out_specs=out_specs,
        scratch_shapes=scratch,
        compiler_params=pltpu.CompilerParams(vmem_limit_bytes=limit * MIB),
    )(*args, *parts)


def per_device(stream, norm_gain, mix_weight, branch_scale):
    rows = stream.shape[0]
    n = NZ * lax.axis_size("tp")
    tail = stream[rows - 2 * HALO :]
    halo = lax.ppermute(tail, ("sp", "tp"), [(i, i + 1) for i in range(n - 1)])
    w0, w1 = gather(mix_weight)
    bf, f32 = jnp.bfloat16, jnp.float32
    shape = jax.ShapeDtypeStruct
    pooled = call(
        pool_kernel, shape((rows + HALO, D), bf), HBM, (halo, norm_gain),
        [pltpu.VMEM((rows, D), bf), pltpu.VMEM((rows + HALO, D), bf), pltpu.VMEM((rows + 2 * HALO, D), bf),
         pltpu.SemaphoreType.DMA((2,))], 24, (), (stream,),
    )
    args = [halo, stream, pooled, branch_scale, norm_gain]
    ext = rows + HALO
    residual, pooled = call(
        middle_kernel, (shape((rows, D), f32), shape((rows, D), bf)), (HBM, VMEM), args,
        [pltpu.VMEM((ext, D), f32), pltpu.VMEM((ext, 128), f32), pltpu.VMEM((ext, 128), f32),
         pltpu.SemaphoreType.DMA((G * NX,))], 40, *w0,
    )
    names, parts = w1
    out = None
    for some in ("ho", "lr"):
        keep = [n for n in names if set(n) & set(some)]
        mine = [v for n, v in zip(names * CORES, parts) if n in keep]
        out = last_call(residual, pooled, branch_scale, tuple(keep), mine, out)
    return out


def solution(mesh):
    return jax.shard_map(
        per_device,
        mesh=mesh,
        in_specs=(P(("grp", "sp", "tp"), None), P(), P(None, None, "sp", "tp"), P()),
        out_specs=P(("grp", "sp", "tp"), None),
        check_vma=False,
    )
```
